32 devices in a mesh: sp: 4 (over z), dp: 8 (over y, x, core).
Axes of the slice: x: 2, y: 2, z: 4, core: 2. Of those that a mesh axis runs over, the one named last changes fastest.
Arguments:
- tokens: bfloat16 [16, 256, 1024], P('dp', 'sp'), may hold values from -6 to 6
- norm_gain: float32 [1024], replicated, may hold values from 0.1 to 1.9
- w_query: bfloat16 [1024, 128], P('dp'), may hold values from -0.1875 to 0.1875
- w_key: bfloat16 [1024, 128], P('dp'), may hold values from -0.1875 to 0.1875
- w_value: bfloat16 [1024, 128], P('dp'), may hold values from -0.1875 to 0.1875
- w_rank_forward: bfloat16 [1024, 16], P('dp'), may hold values from -0.1875 to 0.1875
- w_rank_backward: bfloat16 [1024, 16], P('dp'), may hold values from -0.1875 to 0.1875
- up_forward: bfloat16 [16, 128], replicated, may hold values from -1.5 to 1.5
- up_backward: bfloat16 [16, 128], replicated, may hold values from -1.5 to 1.5
- bias_forward: float32 [128], replicated, may hold values from -1.5 to 3
- bias_backward: float32 [128], replicated, may hold values from -1.5 to 3
- out_gain: float32 [32], replicated, may hold values from 0.1 to 1.9
- w_out: bfloat16 [128, 1024], P('dp'), may hold values from -0.5 to 0.5
Outputs:
- mixed_out: bfloat16 [16, 256, 1024], P('dp', 'sp')
The draws below stay inside these ranges and needn't reach their ends.
All inputs are finite; a program needn't handle non-finite values.
Results may differ from the reference program's by a relative error of at most 0.005.
Values may be sent and summed in bfloat16 or wider, within the bound.
A program may use at most 64 MiB of HBM per device.

```python
import jax
import jax.numpy as jnp
from jax import lax

D = 1024
HK = 32
HV = 32
RANK = 16
BLOCK = 64
SEQS = 16
SEQ = 256
DK = 128
DV = 128


def steps_of(stream_key, shape, split, least, top_value):
    gain = 1.0
    for dim, parts in split:
        draws = jax.random.uniform(jax.random.fold_in(jax.random.fold_in(stream_key, 6), dim), (parts,), jnp.float32, least / len(split), top_value / len(split))
        gain = gain * jnp.repeat(jnp.exp(draws), shape[dim] // parts).reshape((-1,) + (1,) * (len(shape) - 1 - dim))
    return gain


def scatter_about(rng, extent, spread, limit, shards=(), dtype=jnp.bfloat16):
    values = jax.random.normal(rng, extent, jnp.float32) * spread
    if len(shards) > 0:
        values = steps_of(rng, extent, shards, -0.22, 0.18) * values
    return jnp.clip(values, min=-limit, max=limit).astype(dtype)


def setup_inputs(seed: int = 0) -> dict:
    key_of = jax.random.split(jax.random.key(seed), 14)
    tokens = scatter_about(key_of[0], (SEQS, SEQ, D), 1.0, 6.0, ((0, 8), (1, 4)))
    norm_gain = jnp.clip(1.0 + 0.18 * jax.random.normal(key_of[1], (D,), jnp.float32), 0.1, 1.9)
    w_query = scatter_about(key_of[2], (D, DK), D ** -0.5, 0.1875, ((0, 8),))
    w_key = scatter_about(key_of[3], (D, DK), D ** -0.5, 0.1875, ((0, 8),))
    w_value = scatter_about(key_of[4], (D, DV), D ** -0.5, 0.1875, ((0, 8),))
    w_rank_forward = scatter_about(key_of[5], (D, RANK), D ** -0.5, 0.1875, ((0, 8),))
    w_rank_backward = scatter_about(key_of[6], (D, RANK), D ** -0.5, 0.1875, ((0, 8),))
    up_forward = scatter_about(key_of[7], (RANK, DK), RANK ** -0.5, 1.5)
    up_backward = scatter_about(key_of[8], (RANK, DK), RANK ** -0.5, 1.5)
    bias_forward = jnp.clip(jax.random.uniform(key_of[9], (DK,), jnp.float32, -1.5, 3.0), -1.5, 3.0)
    bias_backward = jnp.clip(jax.random.uniform(key_of[10], (DK,), jnp.float32, -1.5, 3.0), -1.5, 3.0)
    out_gain = jnp.clip(1.0 + 0.18 * jax.random.normal(key_of[11], (HV,), jnp.float32), 0.1, 1.9)
    w_out = scatter_about(key_of[12], (DV, D), DV ** -0.5, 0.5, ((0, 8),))
    return dict(tokens=tokens, norm_gain=norm_gain, w_query=w_query, w_key=w_key, w_value=w_value, w_rank_forward=w_rank_forward, w_rank_backward=w_rank_backward, up_forward=up_forward, up_backward=up_backward, bias_forward=bias_forward, bias_backward=bias_backward, out_gain=out_gain, w_out=w_out)


eps = 1e-06
precise = lax.Precision.HIGHEST

def rms_norm(values, norm_scale):
    return values * lax.rsqrt(lax.optimization_barrier(jnp.mean(values * values, axis=-1, keepdims=True)) + eps) * norm_scale

def one_way(queries, key_rows, value_rows, decay_rates):
    head_count, length, key_width = queries.shape
    value_width = value_rows.shape[-1]
    blocks = length // BLOCK

    def in_blocks(tensor):
        return tensor.reshape(head_count, blocks, BLOCK, tensor.shape[-1])
    query_blocks = in_blocks(queries)
    key_blocks = in_blocks(key_rows)
    value_blocks = in_blocks(value_rows)
    running = jnp.cumsum(in_blocks(decay_rates), axis=2)
    closing = running[:, :, -1:, :]
    query_decayed = query_blocks * jnp.exp(running)
    key_inverse = key_blocks * jnp.exp(-running)
    key_remain = key_blocks * jnp.exp(closing - running)
    triangle = jnp.tril(jnp.ones((BLOCK, BLOCK), jnp.float32))
    scores = jnp.einsum('hnid,hnjd->hnij', query_decayed, key_inverse, precision=precise) * triangle
    within = jnp.einsum('hnij,hnjv->hniv', scores, value_blocks, precision=precise)
    block_decay = jnp.exp(closing[:, :, 0, :])

    def advance(carried, inputs):
        query_now, key_now, value_now, decay_now = inputs
        emitted = jnp.einsum('hid,hdv->hiv', query_now, carried, precision=precise)
        carried = decay_now[..., None] * carried + jnp.einsum('hid,hiv->hdv', key_now, value_now, precision=precise)
        return (carried, emitted)
    initial = jnp.zeros((head_count, key_width, value_width), jnp.float32)
    stacked = tuple((jnp.moveaxis(tensor, 1, 0) for tensor in (query_decayed, key_remain, value_blocks, block_decay)))
    final_state, across = lax.scan(advance, initial, stacked)
    return (within + jnp.moveaxis(across, 0, 1)).reshape(head_count, length, value_width)

def both_ways(queries, key_rows, value_rows, rates_forward, rates_backward):
    forward = one_way(queries, key_rows, value_rows, rates_forward)
    backward = one_way(jnp.flip(queries, 1), jnp.flip(key_rows, 1), jnp.flip(value_rows, 1), jnp.flip(rates_backward, 1))
    return forward + jnp.flip(backward, 1)

def by_head(tensor, head_width):
    length = tensor.shape[0]
    return tensor.reshape(length, -1, head_width).transpose(1, 0, 2).astype(jnp.float32)

def attend(queries, key_rows, value_rows, rates_forward, rates_backward, out_gain):
    combined = both_ways(by_head(queries, HK) * HK ** (-0.5), by_head(key_rows, HK), by_head(value_rows, HV), by_head(rates_forward, HK), by_head(rates_backward, HK))
    normed = rms_norm(combined, out_gain).astype(jnp.bfloat16)
    return normed.transpose(1, 0, 2).reshape(normed.shape[1], -1)

def reference(tokens, norm_gain, w_query, w_key, w_value, w_rank_forward, w_rank_backward, up_forward, up_backward, bias_forward, bias_backward, out_gain, w_out):
    rate_scale = 2.0 / SEQ

    def one_sequence(sequence):
        normed = rms_norm(sequence.astype(jnp.float32), norm_gain).astype(jnp.bfloat16)
        queries = jnp.dot(normed, w_query, preferred_element_type=jnp.float32).astype(jnp.bfloat16)
        key_rows = jnp.dot(normed, w_key, preferred_element_type=jnp.float32).astype(jnp.bfloat16)
        value_rows = jnp.dot(normed, w_value, preferred_element_type=jnp.float32).astype(jnp.bfloat16)
        rank_forward = jnp.dot(normed, w_rank_forward, preferred_element_type=jnp.float32).astype(jnp.bfloat16)
        rank_backward = jnp.dot(normed, w_rank_backward, preferred_element_type=jnp.float32).astype(jnp.bfloat16)
        rates_forward = jax.nn.log_sigmoid(jnp.dot(rank_forward, up_forward, preferred_element_type=jnp.float32) + bias_forward) * rate_scale
        rates_backward = jax.nn.log_sigmoid(jnp.dot(rank_backward, up_backward, preferred_element_type=jnp.float32) + bias_backward) * rate_scale
        attended = attend(queries, key_rows, value_rows, rates_forward, rates_backward, out_gain)
        return jnp.dot(attended, w_out, preferred_element_type=jnp.float32).astype(jnp.bfloat16)
    return lax.map(one_sequence, tokens)
```

```python
import functools

import jax
import jax.numpy as jnp
from jax import lax
from jax.experimental import pallas as pl
from jax.experimental.pallas import tpu as pltpu
from jax.sharding import PartitionSpec as P

HK = 32
LANES = 128
EPS = 1e-06
f32 = jnp.float32
bf16 = jnp.bfloat16


def dot(a, b, dims=((1,), (0,))):
    return lax.dot_general(a, b, (dims, ((), ())), preferred_element_type=f32)


def split_dot(a, b):
    high = b.astype(bf16)
    low = (b - high.astype(f32)).astype(bf16)
    return dot(a, high) + dot(a, low)


def kernel(
    n_sp,
    n_dp,
    tokens,
    norm_gain,
    w_query,
    w_key,
    w_value,
    w_rank_f,
    w_rank_b,
    up_f,
    up_b,
    bias_f,
    bias_b,
    out_gain,
    w_out,
    result,
    tok_v,
    gain_v,
    rank_v,
    up_v,
    bias_v,
    ogain_v,
    wr,
    wk,
    wv,
    wq,
    wo,
    states,
    inbox,
    local_sem,
    send_sem,
    relay_sem,
    recv_sem,
    sp_send_sem,
    sp_recv_sem,
):
    sp = lax.axis_index("sp")
    dp = lax.axis_index("dp")
    chips = n_dp // 2
    core = lax.rem(dp, 2)
    chip = lax.div(dp, 2)
    partner = chip * 2 + (1 - core)
    seqs, toks, width = tok_v.shape
    rows = seqs * toks
    depth = w_query.shape[0]
    out_depth = w_out.shape[0]
    keys = w_query.shape[1]
    rank = w_rank_f.shape[1]
    groups = keys // LANES
    heads = LANES // HK

    def slot(which, src):
        ref = (wr, wk, wv, wq, wo)[which]
        if which == 0:
            return ref.at[src]
        size = out_depth if which == 4 else depth
        return ref.at[pl.ds(pl.multiple_of(src * size, size), size), :]

    barrier = pltpu.get_barrier_semaphore()
    far = [lax.rem(chip + s, chips) * 2 + core for s in range(1, chips)]
    peers = [lax.rem(sp + s, n_sp) for s in range(1, n_sp)]
    for d in far + [partner]:
        pl.semaphore_signal(barrier, inc=1, device_id={"dp": d})
    for p in peers:
        pl.semaphore_signal(barrier, inc=1, device_id={"sp": p})

    loads = []
    for src, dst in (
        (w_rank_f, rank_v.at[0]),
        (w_rank_b, rank_v.at[1]),
        (w_key, slot(1, dp)),
        (w_value, slot(2, dp)),
        (w_query, slot(3, dp)),
        (tokens, tok_v),
        (norm_gain, gain_v),
        (w_out, slot(4, dp)),
        (up_f, up_v.at[0]),
        (up_b, up_v.at[1]),
        (bias_f, bias_v.at[0]),
        (bias_b, bias_v.at[1]),
        (out_gain, ogain_v),
    ):
        copy = pltpu.make_async_copy(src, dst, local_sem.at[len(loads)])
        copy.start()
        loads.append(copy)
    inbox[sp] = jnp.zeros(inbox.shape[1:], bf16)
    loads[0].wait()
    loads[1].wait()
    wr[dp] = jnp.concatenate([rank_v[0].astype(f32).T, rank_v[1].astype(f32).T], axis=0).astype(bf16)
    pl.semaphore_wait(barrier, len(far) + 1 + len(peers))

    def remote(which, src, sem, target):
        return pltpu.make_async_remote_copy(
            src_ref=slot(which, src),
            dst_ref=slot(which, src),
            send_sem=sem,
            recv_sem=recv_sem.at[which, src],
            device_id={"dp": target},
        )

    sends = []
    waits = {1: 2, 2: 3, 3: 4, 4: 7}
    for which in range(5):
        if which:
            loads[waits[which]].wait()
        for i, d in enumerate(far):
            copy = remote(which, dp, send_sem.at[which, i], d)
            copy.start()
            sends.append(copy)
        copy = remote(which, dp, relay_sem.at[which, 0], partner)
        copy.start()
        sends.append(copy)

    loads[5].wait()
    loads[6].wait()
    x = tok_v[...].reshape(rows, width).astype(f32)
    normed = (x * lax.rsqrt(jnp.mean(x * x, axis=-1, keepdims=True) + EPS) * gain_v[...]).astype(bf16)

    for copy in loads[8:]:
        copy.wait()

    def relay(which):
        for i in range(1, chips):
            src = lax.rem(chip + chips - i, chips) * 2 + core
            remote(which, src, relay_sem.at[which, i], partner).wait_recv()
            copy = remote(which, src, relay_sem.at[which, i], partner)
            copy.start()
            sends.append(copy)

    def arrive(which):
        for i in range(chips):
            src = lax.rem(chip + chips - i, chips) * 2 + (1 - core)
            remote(which, src, relay_sem.at[which, i], partner).wait_recv()

    row = lax.broadcasted_iota(jnp.int32, (rows, rows), 0)
    col = lax.broadcasted_iota(jnp.int32, (rows, rows), 1)
    same = lax.div(row, toks) == lax.div(col, toks)
    lower = jnp.where(same & (row >= col), 1.0, 0.0).astype(bf16)
    upper = jnp.where(same & (row <= col), 1.0, 0.0).astype(bf16)

    relay(0)
    arrive(0)
    w_ranks = jnp.concatenate([wr[s] for s in range(n_dp)], axis=1)
    ranks = dot(normed, w_ranks, ((1,), (1,))).astype(bf16)
    scale = 2.0 / (toks * n_sp)
    running = []
    for d in range(2):
        logits = dot(ranks[:, d * rank : (d + 1) * rank], up_v[d]) + bias_v[d]
        rates = (jnp.minimum(logits, 0.0) - jnp.log1p(jnp.exp(-jnp.abs(logits)))) * scale
        running.append(split_dot(upper if d else lower, rates))
    relay(1)
    arrive(1)
    k = dot(normed, wk[...]).astype(bf16).astype(f32)
    relay(2)
    arrive(2)
    v = dot(normed, wv[...]).astype(bf16)

    lane = lax.broadcasted_iota(jnp.int32, (1, LANES), 1)
    head_mask = [jnp.where(lax.div(lane, HK) == h, 1.0, 0.0) for h in range(heads)]
    head_mask16 = [m.astype(bf16) for m in head_mask]
    tag_row = lax.broadcasted_iota(jnp.int32, (16, LANES), 0)

    def part(a, b, g):
        return a[b * toks : (b + 1) * toks, g * LANES : (g + 1) * LANES]

    closing = {}
    for b in range(seqs):
        for g in range(groups):
            for d in range(2):
                run = part(running[d], b, g)
                end = run[:1] if d else run[toks - 1 :]
                remain = (part(k, b, g) * jnp.exp(end - run)).astype(bf16)
                summary = dot(remain, part(v, b, g), ((0,), (0,)))
                packed = sum(summary[h * HK : (h + 1) * HK] * head_mask[h] for h in range(heads))
                high = end.astype(bf16).astype(f32)
                tags = jnp.where(tag_row == 0, high, jnp.where(tag_row == 1, end - high, 0.0))
                states[d, b * groups + g] = jnp.concatenate([packed, tags], axis=0).astype(bf16)
    for i, p in enumerate(peers):
        back = jnp.where(p < sp, 1, 0)
        copy = pltpu.make_async_remote_copy(
            src_ref=states.at[back],
            dst_ref=inbox.at[sp],
            send_sem=sp_send_sem.at[i],
            recv_sem=sp_recv_sem.at[sp],
            device_id={"sp": p},
        )
        copy.start()
        sends.append(copy)

    relay(3)
    arrive(3)
    q = dot(normed, wq[...]).astype(bf16).astype(f32) * HK ** (-0.5)
    relay(4)

    t_row = lax.broadcasted_iota(jnp.int32, (toks, heads * toks), 0)
    t_col = lax.rem(lax.broadcasted_iota(jnp.int32, (toks, heads * toks), 1), toks)
    decayed = {}
    inner = {}
    for b in range(seqs):
        for g in range(groups):
            scores = 0.0
            for d in range(2):
                run = part(running[d], b, g)
                qd = part(q, b, g) * jnp.exp(run)
                ki = part(k, b, g) * jnp.exp(-run)
                decayed[b, g, d] = qd
                stack = jnp.concatenate([(ki * m).astype(bf16) for m in head_mask], axis=0)
                s = dot(qd.astype(bf16), stack, ((1,), (1,)))
                keep = t_row <= t_col if d else t_row >= t_col
                scores = scores + jnp.where(keep, s, 0.0)
            vb = part(v, b, g)
            v_stack = jnp.concatenate([vb * m for m in head_mask16], axis=0)
            inner[b, g] = dot(scores.astype(bf16), v_stack)

    for i in range(1, n_sp):
        src = lax.rem(sp + n_sp - i, n_sp)
        pltpu.make_async_remote_copy(
            src_ref=states.at[0],
            dst_ref=inbox.at[src],
            send_sem=sp_send_sem.at[i - 1],
            recv_sem=sp_recv_sem.at[src],
            device_id={"sp": src},
        ).wait_recv()

    block_row = lax.div(lax.broadcasted_iota(jnp.int32, (LANES, LANES), 0), HK)
    block_col = lax.div(lax.broadcasted_iota(jnp.int32, (LANES, LANES), 1), HK)
    block_ones = jnp.where(block_row == block_col, 1.0, 0.0).astype(bf16)
    gain = jnp.concatenate([ogain_v[...]] * heads, axis=1)
    attended = []
    for b in range(seqs):
        per_group = []
        for g in range(groups):
            box = [inbox[i, b * groups + g] for i in range(n_sp)]
            ends = [
                box[i][HK : HK + 1].astype(f32) + box[i][HK + 1 : HK + 2].astype(f32)
                for i in range(n_sp)
            ]
            between = [None] * n_sp
            run_f = jnp.zeros((1, LANES), f32)
            run_b = jnp.zeros((1, LANES), f32)
            pre_f = [None] * n_sp
            pre_b = [None] * n_sp
            for i in reversed(range(n_sp)):
                pre_f[i] = run_f
                run_f = run_f + jnp.where(sp > i, 1.0, 0.0) * ends[i]
            for i in range(n_sp):
                pre_b[i] = run_b
                run_b = run_b + jnp.where(sp < i, 1.0, 0.0) * ends[i]
            queries = []
            memory = []
            for i in range(n_sp):
                first = sp > i
                factor = jnp.exp(jnp.where(first, pre_f[i], pre_b[i]))
                base = jnp.where(first, decayed[b, g, 0], decayed[b, g, 1])
                queries.append((base * factor).astype(bf16))
                packed = box[i][:HK]
                memory += [packed * m for m in head_mask16]
            across = dot(jnp.concatenate(queries, axis=1), jnp.concatenate(memory, axis=0))
            out = inner[b, g] + across
            square = out * out
            high = square.astype(bf16)
            low = (square - high.astype(f32)).astype(bf16)
            mean = (dot(high, block_ones) + dot(low, block_ones)) * (1.0 / HK)
            per_group.append((out * lax.rsqrt(mean + EPS) * gain).astype(bf16))
        attended.append(jnp.concatenate(per_group, axis=1))
    arrive(4)
    mixed = dot(jnp.concatenate(attended, axis=0), wo[...]).astype(bf16)
    result[...] = mixed.reshape(seqs, toks, width)
    for copy in sends:
        copy.wait_send()


def solution(mesh):
    n_sp = mesh.shape["sp"]
    n_dp = mesh.shape["dp"]
    chips = n_dp // 2

    def per_device(
        tokens,
        norm_gain,
        w_query,
        w_key,
        w_value,
        w_rank_forward,
        w_rank_backward,
        up_forward,
        up_backward,
        bias_forward,
        bias_backward,
        out_gain,
        w_out,
    ):
        seqs, toks, width = tokens.shape
        depth, keys = w_query.shape
        rank = w_rank_forward.shape[1]
        groups = keys // LANES
        out_depth = w_out.shape[0]
        anywhere = pl.BlockSpec(memory_space=pl.ANY)
        return pl.pallas_call(
            functools.partial(kernel, n_sp, n_dp),
            out_shape=jax.ShapeDtypeStruct(tokens.shape, bf16),
            in_specs=[anywhere] * 13,
            out_specs=pl.BlockSpec(memory_space=pltpu.VMEM),
            scratch_shapes=[
                pltpu.VMEM((seqs, toks, width), bf16),
                pltpu.VMEM((1, width), f32),
                pltpu.VMEM((2, depth, rank), bf16),
                pltpu.VMEM((2, rank, keys), bf16),
                pltpu.VMEM((2, 1, keys), f32),
                pltpu.VMEM((1, HK), f32),
                pltpu.VMEM((n_dp, 2 * rank, depth), bf16),
                pltpu.VMEM((n_dp * depth, keys), bf16),
                pltpu.VMEM((n_dp * depth, keys), bf16),
                pltpu.VMEM((n_dp * depth, keys), bf16),
                pltpu.VMEM((n_dp * out_depth, width), bf16),
                pltpu.VMEM((2, seqs * groups, HK + 16, LANES), bf16),
                pltpu.VMEM((n_sp, seqs * groups, HK + 16, LANES), bf16),
                pltpu.SemaphoreType.DMA((13,)),
                pltpu.SemaphoreType.DMA((5, chips - 1)),
                pltpu.SemaphoreType.DMA((5, chips)),
                pltpu.SemaphoreType.DMA((5, n_dp)),
                pltpu.SemaphoreType.DMA((n_sp - 1,)),
                pltpu.SemaphoreType.DMA((n_sp,)),
            ],
            compiler_params=pltpu.CompilerParams(collective_id=0, has_side_effects=True),
        )(
            tokens,
            norm_gain.reshape(1, -1),
            w_query,
            w_key,
            w_value,
            w_rank_forward,
            w_rank_backward,
            up_forward,
            up_backward,
            bias_forward.reshape(1, -1),
            bias_backward.reshape(1, -1),
            out_gain.reshape(1, -1),
            w_out,
        )

    rows = P("dp", None)
    return jax.shard_map(
        per_device,
        mesh=mesh,
        in_specs=(P("dp", "sp", None), P(), rows, rows, rows, rows, rows, P(), P(), P(), P(), P(), rows),
        out_specs=P("dp", "sp", None),
        check_vma=False,
    )
```

```python
import functools

import jax
import jax.numpy as jnp
from jax import lax
from jax.experimental import pallas as pl
from jax.experimental.pallas import tpu as pltpu
from jax.sharding import PartitionSpec as P

HK = 32
LANES = 128
TAGS = 8
EPS = 1e-06
f32 = jnp.float32
bf16 = jnp.bfloat16


def dot(a, b, dims=((1,), (0,))):
    return lax.dot_general(a, b, (dims, ((), ())), preferred_element_type=f32)


def in_two(a):
    high = a.astype(bf16)
    return high, (a - high.astype(f32)).astype(bf16)


def split_dot(a, b):
    high, low = in_two(b)
    return dot(a, high) + dot(a, low)


def kernel(
    n_sp,
    n_dp,
    tokens,
    norm_gain,
    w_query,
    w_key,
    w_value,
    w_rank_f,
    w_rank_b,
    up_f,
    up_b,
    bias_f,
    bias_b,
    out_gain,
    w_out,
    result,
    tok_v,
    gain_v,
    up_v,
    bias_v,
    ogain_v,
    wr,
    wk,
    wv,
    wq,
    wo,
    states,
    inbox,
    local_sem,
    send_sem,
    relay_sem,
    recv_sem,
    sp_send_sem,
    sp_recv_sem,
):
    sp = lax.axis_index("sp")
    dp = lax.axis_index("dp")
    chips = n_dp // 2
    core = lax.rem(dp, 2)
    chip = lax.div(dp, 2)
    partner = chip * 2 + (1 - core)
    seqs, toks, width = tok_v.shape
    rows = seqs * toks
    depth = w_query.shape[0]
    out_depth = w_out.shape[0]
    keys = w_query.shape[1]
    rank = w_rank_f.shape[0]
    groups = keys // LANES
    heads = LANES // HK

    def slot(which, src):
        ref = (wr, wk, wv, wq, wo)[which]
        if which == 0:
            return ref.at[src]
        size = out_depth if which == 4 else depth
        return ref.at[pl.ds(pl.multiple_of(src * size, size), size), :]

    barrier = pltpu.get_barrier_semaphore()
    far = [lax.rem(chip + s, chips) * 2 + core for s in range(1, chips)]
    peers = [lax.rem(sp + s, n_sp) for s in range(1, n_sp)]
    for d in far + [partner]:
        pl.semaphore_signal(barrier, inc=1, device_id={"dp": d})
    for p in peers:
        pl.semaphore_signal(barrier, inc=1, device_id={"sp": p})

    loads = []
    for src, dst in (
        (w_rank_f, wr.at[dp, pl.ds(0, rank)]),
        (w_rank_b, wr.at[dp, pl.ds(rank, rank)]),
        (w_key, slot(1, dp)),
        (w_value, slot(2, dp)),
        (w_query, slot(3, dp)),
        (tokens, tok_v),
        (norm_gain, gain_v),
        (w_out, slot(4, dp)),
        (up_f, up_v.at[0]),
        (up_b, up_v.at[1]),
        (bias_f, bias_v.at[0]),
        (bias_b, bias_v.at[1]),
        (out_gain, ogain_v),
    ):
        copy = pltpu.make_async_copy(src, dst, local_sem.at[len(loads)])
        copy.start()
        loads.append(copy)
    inbox[sp] = jnp.zeros(inbox.shape[1:], bf16)
    loads[0].wait()
    loads[1].wait()
    pl.semaphore_wait(barrier, len(far) + 1 + len(peers))

    def remote(which, src, sem, target):
        return pltpu.make_async_remote_copy(
            src_ref=slot(which, src),
            dst_ref=slot(which, src),
            send_sem=sem,
            recv_sem=recv_sem.at[which, src],
            device_id={"dp": target},
        )

    sends = []
    waits = {1: 2, 2: 3, 3: 4, 4: 7}
    for which in range(5):
        if which:
            loads[waits[which]].wait()
        for i, d in enumerate(far):
            copy = remote(which, dp, send_sem.at[which, i], d)
            copy.start()
            sends.append(copy)
        copy = remote(which, dp, relay_sem.at[which, 0], partner)
        copy.start()
        sends.append(copy)

    loads[5].wait()
    loads[6].wait()
    x = tok_v[...].reshape(rows, width).astype(f32)
    normed = (x * lax.rsqrt(jnp.mean(x * x, axis=-1, keepdims=True) + EPS) * gain_v[...]).astype(bf16)

    for copy in loads[8:]:
        copy.wait()

    def relay(which):
        for i in range(1, chips):
            src = lax.rem(chip + chips - i, chips) * 2 + core
            remote(which, src, relay_sem.at[which, i], partner).wait_recv()
            copy = remote(which, src, relay_sem.at[which, i], partner)
            copy.start()
            sends.append(copy)

    def arrive(which):
        for i in range(chips):
            src = lax.rem(chip + chips - i, chips) * 2 + (1 - core)
            remote(which, src, relay_sem.at[which, i], partner).wait_recv()

    row = lax.broadcasted_iota(jnp.int32, (rows, rows), 0)
    col = lax.broadcasted_iota(jnp.int32, (rows, rows), 1)
    same = lax.div(row, toks) == lax.div(col, toks)
    lower = jnp.where(same & (row >= col), 1.0, 0.0).astype(bf16)
    upper = jnp.where(same & (row <= col), 1.0, 0.0).astype(bf16)

    relay(0)
    relay(1)
    arrive(0)
    w_ranks = jnp.concatenate([wr[s] for s in range(n_dp)], axis=1)
    ranks = dot(normed, w_ranks, ((1,), (1,))).astype(bf16)
    scale = 2.0 / (toks * n_sp)
    running = []
    for d in range(2):
        logits = dot(ranks[:, d * rank : (d + 1) * rank], up_v[d]) + bias_v[d]
        rates = (jnp.minimum(logits, 0.0) - jnp.log1p(jnp.exp(-jnp.abs(logits)))) * scale
        running.append(split_dot(upper if d else lower, rates))
    relay(2)
    arrive(1)
    k = dot(normed, wk[...]).astype(bf16).astype(f32)

    def part(a, b, g):
        return a[b * toks : (b + 1) * toks, g * LANES : (g + 1) * LANES]

    remain = {}
    ends = {}
    for b in range(seqs):
        for g in range(groups):
            for d in range(2):
                run = part(running[d], b, g)
                end = run[:1] if d else run[toks - 1 :]
                ends[b, g, d] = end
                remain[b, g, d] = (part(k, b, g) * jnp.exp(end - run)).astype(bf16)
    arrive(2)
    v = dot(normed, wv[...]).astype(bf16)

    lane = lax.broadcasted_iota(jnp.int32, (1, LANES), 1)
    head_mask = [jnp.where(lax.div(lane, HK) == h, 1.0, 0.0) for h in range(heads)]
    head_mask16 = [m.astype(bf16) for m in head_mask]
    tag_row = lax.broadcasted_iota(jnp.int32, (TAGS, LANES), 0)

    for b in range(seqs):
        for g in range(groups):
            for d in range(2):
                end = ends[b, g, d]
                summary = dot(remain[b, g, d], part(v, b, g), ((0,), (0,)))
                packed = sum(summary[h * HK : (h + 1) * HK] * head_mask[h] for h in range(heads))
                high = end.astype(bf16).astype(f32)
                tags = jnp.where(tag_row == 0, high, jnp.where(tag_row == 1, end - high, 0.0))
                states[d, b * groups + g] = jnp.concatenate([packed, tags], axis=0).astype(bf16)
    for i, p in enumerate(peers):
        back = jnp.where(p < sp, 1, 0)
        copy = pltpu.make_async_remote_copy(
            src_ref=states.at[back],
            dst_ref=inbox.at[sp],
            send_sem=sp_send_sem.at[i],
            recv_sem=sp_recv_sem.at[sp],
            device_id={"sp": p},
        )
        copy.start()
        sends.append(copy)

    relay(3)
    arrive(3)
    q = dot(normed, wq[...]).astype(bf16).astype(f32) * HK ** (-0.5)
    relay(4)

    t_row = lax.broadcasted_iota(jnp.int32, (toks, heads * toks), 0)
    t_col = lax.rem(lax.broadcasted_iota(jnp.int32, (toks, heads * toks), 1), toks)
    decayed = {}
    inner = {}
    for b in range(seqs):
        for g in range(groups):
            scores = 0.0
            for d in range(2):
                run = part(running[d], b, g)
                qd = part(q, b, g) * jnp.exp(run)
                ki = part(k, b, g) * jnp.exp(-run)
                decayed[b, g, d] = qd
                q_high, q_low = in_two(qd)
                k_high, k_low = in_two(ki)
                high = jnp.concatenate([k_high * m for m in head_mask16], axis=0)
                low = jnp.concatenate([k_low * m for m in head_mask16], axis=0)
                s = dot(
                    jnp.concatenate([q_high, q_low, q_high], axis=1),
                    jnp.concatenate([high, high, low], axis=1),
                    ((1,), (1,)),
                )
                keep = t_row <= t_col if d else t_row >= t_col
                scores = scores + jnp.where(keep, s, 0.0)
            vb = part(v, b, g)
            v_stack = jnp.concatenate([vb * m for m in head_mask16], axis=0)
            s_high, s_low = in_two(scores)
            inner[b, g] = dot(s_high, v_stack) + dot(s_low, v_stack)

    for i in range(1, n_sp):
        src = lax.rem(sp + n_sp - i, n_sp)
        pltpu.make_async_remote_copy(
            src_ref=states.at[0],
            dst_ref=inbox.at[src],
            send_sem=sp_send_sem.at[i - 1],
            recv_sem=sp_recv_sem.at[src],
            device_id={"sp": src},
        ).wait_recv()

    block_row = lax.div(lax.broadcasted_iota(jnp.int32, (LANES, LANES), 0), HK)
    block_col = lax.div(lax.broadcasted_iota(jnp.int32, (LANES, LANES), 1), HK)
    block_ones = jnp.where(block_row == block_col, 1.0, 0.0).astype(bf16)
    gain = jnp.concatenate([ogain_v[...]] * heads, axis=1)
    attended = []
    for b in range(seqs):
        per_group = []
        for g in range(groups):
            box = [inbox[i, b * groups + g] for i in range(n_sp)]
            tails = [
                box[i][HK : HK + 1].astype(f32) + box[i][HK + 1 : HK + 2].astype(f32)
                for i in range(n_sp)
            ]
            run_f = jnp.zeros((1, LANES), f32)
            run_b = jnp.zeros((1, LANES), f32)
            pre_f = [None] * n_sp
            pre_b = [None] * n_sp
            for i in reversed(range(n_sp)):
                pre_f[i] = run_f
                run_f = run_f + jnp.where(sp > i, 1.0, 0.0) * tails[i]
            for i in range(n_sp):
                pre_b[i] = run_b
                run_b = run_b + jnp.where(sp < i, 1.0, 0.0) * tails[i]
            queries = []
            memory = []
            for i in range(n_sp):
                first = sp > i
                factor = jnp.exp(jnp.where(first, pre_f[i], pre_b[i]))
                base = jnp.where(first, decayed[b, g, 0], decayed[b, g, 1])
                queries.append((base * factor).astype(bf16))
                packed = box[i][:HK]
                memory += [packed * m for m in head_mask16]
            across = dot(jnp.concatenate(queries, axis=1), jnp.concatenate(memory, axis=0))
            out = inner[b, g] + across
            square = out * out
            high = square.astype(bf16)
            low = (square - high.astype(f32)).astype(bf16)
            mean = (dot(high, block_ones) + dot(low, block_ones)) * (1.0 / HK)
            per_group.append((out * lax.rsqrt(mean + EPS) * gain).astype(bf16))
        attended.append(jnp.concatenate(per_group, axis=1))
    arrive(4)
    mixed = dot(jnp.concatenate(attended, axis=0), wo[...]).astype(bf16)
    result[...] = mixed.reshape(seqs, toks, width)
    for copy in sends:
        copy.wait_send()


def solution(mesh):
    n_sp = mesh.shape["sp"]
    n_dp = mesh.shape["dp"]
    chips = n_dp // 2

    def per_device(
        tokens,
        norm_gain,
        w_query,
        w_key,
        w_value,
        w_rank_forward,
        w_rank_backward,
        up_forward,
        up_backward,
        bias_forward,
        bias_backward,
        out_gain,
        w_out,
    ):
        seqs, toks, width = tokens.shape
        depth, keys = w_query.shape
        rank = w_rank_forward.shape[1]
        groups = keys // LANES
        out_depth = w_out.shape[0]
        anywhere = pl.BlockSpec(memory_space=pl.ANY)
        return pl.pallas_call(
            functools.partial(kernel, n_sp, n_dp),
            out_shape=jax.ShapeDtypeStruct(tokens.shape, bf16),
            in_specs=[anywhere] * 13,
            out_specs=pl.BlockSpec(memory_space=pltpu.VMEM),
            scratch_shapes=[
                pltpu.VMEM((seqs, toks, width), bf16),
                pltpu.VMEM((1, width), f32),
                pltpu.VMEM((2, rank, keys), bf16),
                pltpu.VMEM((2, 1, keys), f32),
                pltpu.VMEM((1, HK), f32),
                pltpu.VMEM((n_dp, 2 * rank, depth), bf16),
                pltpu.VMEM((n_dp * depth, keys), bf16),
                pltpu.VMEM((n_dp * depth, keys), bf16),
                pltpu.VMEM((n_dp * depth, keys), bf16),
                pltpu.VMEM((n_dp * out_depth, width), bf16),
                pltpu.VMEM((2, seqs * groups, HK + TAGS, LANES), bf16),
                pltpu.VMEM((n_sp, seqs * groups, HK + TAGS, LANES), bf16),
                pltpu.SemaphoreType.DMA((13,)),
                pltpu.SemaphoreType.DMA((5, chips - 1)),
                pltpu.SemaphoreType.DMA((5, chips)),
                pltpu.SemaphoreType.DMA((5, n_dp)),
                pltpu.SemaphoreType.DMA((n_sp - 1,)),
                pltpu.SemaphoreType.DMA((n_sp,)),
            ],
            compiler_params=pltpu.CompilerParams(collective_id=0, has_side_effects=True),
        )(
            tokens,
            norm_gain.reshape(1, -1),
            w_query,
            w_key,
            w_value,
            w_rank_forward.T,
            w_rank_backward.T,
            up_forward,
            up_backward,
            bias_forward.reshape(1, -1),
            bias_backward.reshape(1, -1),
            out_gain.reshape(1, -1),
            w_out,
        )

    rows = P("dp", None)
    return jax.shard_map(
        per_device,
        mesh=mesh,
        in_specs=(P("dp", "sp", None), P(), rows, rows, rows, rows, rows, P(), P(), P(), P(), P(), rows),
        out_specs=P("dp", "sp", None),
        check_vma=False,
    )
```
